32 devices in a mesh: sp: 8 (over z, y), tp: 4 (over x, core).
Axes of the slice: x: 2, y: 2, z: 4, core: 2. Of those that a mesh axis runs over, the one named last changes fastest.
Arguments:
- stream: bfloat16 [2048, 2048], P('sp', 'tp'), may hold values from -8 to 8
- norm_gain: float32 [2, 2048], P(None, 'tp'), may hold values from 0.1 to 1.9
- query_weight: bfloat16 [2, 2048, 1024], P(None, None, 'tp'), may hold values from -4 to 4
- key_weight: bfloat16 [2, 2048, 1024], P(None, None, 'tp'), may hold values from -4 to 4
- value_weight: bfloat16 [2, 2048, 1024], P(None, None, 'tp'), may hold values from -0.125 to 0.125
- out_weight: bfloat16 [2, 1024, 2048], P(None, None, 'tp'), may hold values from -1.5 to 1.5
- rel_bias: float32 [2, 16, 257], P(None, 'tp'), may hold values from -4 to 4
Outputs:
- mixed: bfloat16 [2048, 2048], P('sp', 'tp')
The draws below stay inside these ranges and needn't reach their ends.
All inputs are finite; a program needn't handle non-finite values.
Results may differ from the reference program's by a relative error of at most 0.013.
Values may be sent and summed in bfloat16 or wider, within the bound.
A program may use at most 64 MiB of HBM per device.

```python
import math
import jax
import jax.numpy as jnp
from jax import lax

D = 2048
HEADS = 16
HEAD_DIM = 64
SEG = 64
PREV = 8
CLIP = 128
LAYERS = 2
TOKENS = 2048


def paired_weights(key):
    base_key = jax.random.fold_in(key, 7001)
    shape = (LAYERS, D, HEADS * HEAD_DIM)
    query_part = jax.random.normal(jax.random.fold_in(base_key, 1), shape, jnp.float32) * D ** (-0.5)
    other_part = jax.random.normal(jax.random.fold_in(base_key, 2), shape, jnp.float32) * D ** (-0.5)
    key_part = other_part
    return (jnp.clip(query_part, -4.0, 4.0), jnp.clip(key_part, -4.0, 4.0))


def draw_query_weight(key, part):
    return paired_weights(key)[0].astype(jnp.bfloat16)


def draw_key_weight(key, part):
    return paired_weights(key)[1].astype(jnp.bfloat16)


def draw_stream(key, part):
    ramp = jnp.exp(jnp.linspace(math.log(0.5), math.log(2.0), D, dtype=jnp.float32))
    jitter = jnp.exp(jax.random.uniform(jax.random.fold_in(key, 5005), (D,), jnp.float32, -0.35, 0.35))
    column_scale = (ramp * jitter)[None, :]
    base_rows = jnp.clip(jax.random.normal(jax.random.fold_in(key, 5001), (TOKENS, D), jnp.float32), -6.0, 6.0)
    return jnp.clip(base_rows * column_scale, -8.0, 8.0).astype(jnp.bfloat16)


def level_of(rng, dims, cuts, least, largest):
    def one(position, parts):
        steps = jax.random.uniform(jax.random.fold_in(jax.random.fold_in(rng, 6), position), (parts,), jnp.float32, least / len(cuts), largest / len(cuts))
        return jnp.repeat(jnp.exp(steps), dims[position] // parts).reshape((-1,) + (1,) * (len(dims) - position - 1))

    factor_of = one(*cuts[0])
    for cut in cuts[1:]:
        factor_of = factor_of * one(*cut)
    return factor_of


def scatter_about(key, extent, spread, limit, shards=(), kind=jnp.bfloat16):
    result = spread * jax.random.normal(key, extent, jnp.float32)
    if shards:
        result = result * level_of(key, extent, shards, -0.22, 0.18)
    return jnp.clip(result, -limit, limit).astype(kind)


def setup_inputs(seed: int = 0) -> dict:
    keys = jax.random.split(jax.random.key(seed), 8)
    stream = draw_stream(jax.random.fold_in(keys[7], 71), 0)
    norm_gain = jnp.clip(1.0 + 0.18 * jax.random.normal(keys[1], (LAYERS, D), jnp.float32), 0.1, 1.9)
    query_weight = draw_query_weight(jax.random.fold_in(keys[7], 71), 0)
    key_weight = draw_key_weight(jax.random.fold_in(keys[7], 71), 0)
    value_weight = scatter_about(keys[4], (LAYERS, D, HEADS * HEAD_DIM), D ** -0.5, 0.125, ((2, 4),))
    out_weight = scatter_about(keys[5], (LAYERS, HEADS * HEAD_DIM, D), (HEADS * HEAD_DIM // 64) ** -0.5, 1.5, ((2, 4),))
    rel_bias = scatter_about(keys[6], (LAYERS, HEADS, 2 * CLIP + 1), 1.0, 4.0, ((1, 4),), jnp.float32)
    return dict(stream=stream, norm_gain=norm_gain, query_weight=query_weight, key_weight=key_weight, value_weight=value_weight, out_weight=out_weight, rel_bias=rel_bias)


epsilon = 1e-06
masked_score = -1e+30

def normalize(residual, gain):
    values_f = residual.astype(jnp.float32)
    scaled = values_f * lax.rsqrt(lax.optimization_barrier(jnp.mean(values_f * values_f, axis=-1, keepdims=True)) + epsilon)
    return (scaled * gain).astype(jnp.bfloat16)

def distance_index(band_len):
    within = jnp.arange(SEG, dtype=jnp.int32)[:, None]
    across = jnp.arange(band_len, dtype=jnp.int32)[None, :]
    return jnp.minimum(band_len - SEG + within - across, CLIP) + CLIP

def reference(stream, norm_gain, query_weight, key_weight, value_weight, out_weight, rel_bias):
    reach_rows = PREV * SEG
    band_len = reach_rows + SEG
    head_cols = HEADS * HEAD_DIM
    table_index = distance_index(band_len)
    residual = stream
    for layer_index in range(LAYERS):
        normed = normalize(residual, norm_gain[layer_index])
        query_rows = jnp.dot(normed, query_weight[layer_index], preferred_element_type=jnp.float32).astype(jnp.bfloat16)
        key_rows = jnp.dot(normed, key_weight[layer_index], preferred_element_type=jnp.float32).astype(jnp.bfloat16)
        value_rows = jnp.dot(normed, value_weight[layer_index], preferred_element_type=jnp.float32).astype(jnp.bfloat16)
        padding = jnp.zeros((reach_rows, head_cols), jnp.bfloat16)
        key_ext = jnp.concatenate([padding, key_rows], axis=0)
        value_ext = jnp.concatenate([padding, value_rows], axis=0)
        position_bias = rel_bias[layer_index][:, table_index]

        def one_segment(segment):
            start = (segment * SEG).astype(jnp.int32)
            queries = lax.dynamic_slice_in_dim(query_rows, start, SEG, 0).astype(jnp.float32).reshape(SEG, HEADS, HEAD_DIM)
            keys_band = lax.dynamic_slice_in_dim(key_ext, start, band_len, 0).astype(jnp.float32).reshape(band_len, HEADS, HEAD_DIM)
            values_band = lax.dynamic_slice_in_dim(value_ext, start, band_len, 0).astype(jnp.float32).reshape(band_len, HEADS, HEAD_DIM)
            visible = start - reach_rows + jnp.arange(band_len, dtype=jnp.int32) >= 0
            scores = jnp.einsum('qhd,khd->hqk', queries, keys_band) * HEAD_DIM ** (-0.5) + position_bias
            scores = jnp.where(visible[None, None, :], scores, masked_score)
            maximum = lax.optimization_barrier(jnp.max(scores, axis=-1, keepdims=True))
            exponent = jnp.exp(scores - maximum)
            weights = (exponent / lax.optimization_barrier(jnp.sum(exponent, axis=-1, keepdims=True))).astype(jnp.bfloat16)
            attended = jnp.einsum('hqk,khd->qhd', weights.astype(jnp.float32), values_band)
            return attended.astype(jnp.bfloat16).reshape(SEG, head_cols)
        attended = lax.map(one_segment, jnp.arange(TOKENS // SEG, dtype=jnp.int32)).reshape(TOKENS, head_cols)
        total = jnp.dot(attended, out_weight[layer_index], preferred_element_type=jnp.float32)
        residual = (residual.astype(jnp.float32) + total).astype(jnp.bfloat16)
    return residual
```

```python
import functools

import jax
import jax.numpy as jnp
from jax import lax
from jax.experimental import pallas as pl
from jax.experimental.pallas import tpu as pltpu
from jax.sharding import PartitionSpec as P

SEG = 64
PREV = 8
CLIP = 128
LANES = 128
CHUNKS = 4
DIRECT = 1
PAIR = 2 * SEG
REACH = PREV * SEG
BAND = REACH + PAIR

epsilon = 1e-06
masked_score = -1e30
MESH = pl.DeviceIdType.MESH


class Gather:
    def __init__(self, n_tp, slot, send_sems, recv_sems):
        self.n_x = n_tp // 2
        self.me = lax.axis_index("tp")
        self.core = lax.rem(self.me, 2)
        self.x = self.me // 2
        self.sibling = self.me + 1 - 2 * self.core
        self.slot, self.send_sems, self.recv_sems = slot, send_sems, recv_sems

    def across(self, step, core):
        return lax.rem(self.x + step, self.n_x) * 2 + core

    def copy(self, source, origin, part, index, target):
        return pltpu.make_async_remote_copy(
            src_ref=source,
            dst_ref=self.slot(origin, part),
            send_sem=self.send_sems.at[part, index],
            recv_sem=self.recv_sems.at[part, origin],
            device_id={"tp": target},
            device_id_type=MESH,
        )

    def own(self, part, source=None):
        source = self.slot(self.me, part) if source is None else source
        targets = [self.across(s, self.core) for s in range(1, self.n_x)] + [self.sibling]
        return [self.copy(source, self.me, part, i, t) for i, t in enumerate(targets)]

    def send(self, part, source=None):
        for copy in self.own(part, source):
            copy.start()

    def relays(self, part):
        out = []
        for s in range(1, self.n_x):
            origin = self.across(s, self.core)
            out.append(
                self.copy(self.slot(origin, part), origin, part, self.n_x - 1 + s, self.sibling)
            )
        return out

    def relay(self, part):
        for copy in self.relays(part):
            copy.wait_recv()
            copy.start()

    def others(self):
        return [self.sibling] + [self.across(s, 1 - self.core) for s in range(1, self.n_x)]

    def wait_slot(self, part, origin):
        self.copy(self.slot(origin, part), origin, part, 0, self.sibling).wait_recv()

    def wait_rest(self, part):
        for origin in self.others():
            self.wait_slot(part, origin)

    def finish(self, part, source=None):
        for copy in self.own(part, source) + self.relays(part):
            copy.wait_send()


def kernel(
    n_tp, n_sp, head_dim,
    stream, gain, query_w, key_w, value_w, out_w, rel_bias,
    out,
    xg, gg, table, wkv, wq, wo, normed, bias, edge, qx, kvx, att, top_s, sum_s, mix_s,
    xs, xr, ats, atr, kvs, kvr, gs, gr, wsem, own_sem,
):
    layers, _, rows, width = xg.shape
    head_cols = qx.shape[1]
    groups = head_cols // LANES
    per_group = LANES // head_dim
    total_width = n_tp * width
    shift = REACH // rows
    sp = lax.axis_index("sp")
    tp = lax.axis_index("tp")
    core = lax.rem(tp, 2)
    relayed = shift == 2 and n_sp % 2 == 0
    blocks = rows // PAIR
    piece = rows // CHUNKS
    per_block = CHUNKS // blocks
    heads = per_group * groups
    tall = per_group * PAIR

    key_cols, value_cols = slice(0, head_cols), slice(head_cols, 2 * head_cols)
    weights = []
    for l in range(layers):
        pairs = (
            (key_w, wkv.at[l, :, key_cols]),
            (value_w, wkv.at[l, :, value_cols]),
            (query_w, wq.at[l]),
            (out_w, wo.at[l]),
        )
        weights.append(
            [pltpu.make_async_copy(s.at[l], d, wsem.at[l, i]) for i, (s, d) in enumerate(pairs)]
        )
    own_stream = pltpu.make_async_copy(stream, xg.at[0, tp], own_sem.at[0])
    own_gain = pltpu.make_async_copy(gain, gg.at[tp], own_sem.at[1])
    own_stream.start()
    own_gain.start()
    own_table = pltpu.make_async_copy(rel_bias, table, own_sem.at[2])
    own_table.start()

    barrier = pltpu.get_barrier_semaphore()
    for d in range(1, n_tp):
        pl.semaphore_signal(
            barrier, inc=1, device_id={"tp": lax.rem(tp + d, n_tp)}, device_id_type=MESH
        )
    count = n_tp - 1
    for d in range(1, shift + 1):

        @pl.when(sp + d < n_sp)
        def _():
            pl.semaphore_signal(barrier, inc=1, device_id={"sp": sp + d}, device_id_type=MESH)

        @pl.when(sp >= d)
        def _():
            pl.semaphore_signal(barrier, inc=1, device_id={"sp": sp - d}, device_id_type=MESH)

        count = count + jnp.where(sp + d < n_sp, 1, 0) + jnp.where(sp >= d, 1, 0)
    for copy in weights[0]:
        copy.start()
    with jax.named_scope("barrier"):
        pl.semaphore_wait(barrier, count)

    xgather = [
        Gather(
            n_tp,
            lambda j, c, l=l: xg.at[l, j, pl.ds(c * piece, piece)],
            xs.at[l],
            xr.at[l],
        )
        for l in range(layers)
    ]
    agather = [
        Gather(n_tp, lambda j, p, l=l: att.at[l, j, p], ats.at[l], atr.at[l])
        for l in range(layers)
    ]

    own_stream.wait()
    for c in range(CHUNKS):
        xgather[0].send(c)
    gain_copies = [
        pltpu.make_async_remote_copy(
            src_ref=gain,
            dst_ref=gg.at[tp],
            send_sem=gs.at[d - 1],
            recv_sem=gr.at[d - 1],
            device_id={"tp": lax.rem(tp + d, n_tp)},
            device_id_type=MESH,
        )
        for d in range(1, n_tp)
    ]
    for copy in gain_copies:
        copy.start()
    for l in range(1, layers):
        for copy in weights[l]:
            copy.start()

    for l in range(layers):
        for d in range(1, shift + 1):

            @pl.when(sp < d)
            def _():
                kvx[l, pl.ds((shift - d) * rows, rows), :] = jnp.zeros(
                    (rows, 2 * head_cols), jnp.bfloat16
                )

    near = 2 * CLIP

    def make_bias():
        own_table.wait()
        flip = (
            lax.broadcasted_iota(jnp.int32, (near, near), 0)
            + lax.broadcasted_iota(jnp.int32, (near, near), 1)
            == near - 1
        ).astype(jnp.float32)
        q_row = lax.broadcasted_iota(jnp.int32, (PAIR, PAIR), 0)
        k_col = lax.broadcasted_iota(jnp.int32, (PAIR, PAIR), 1)
        later = (q_row < SEG) & (k_col >= SEG)
        before = (q_row >= SEG) & (k_col < SEG)
        far_hidden = jnp.where(sp >= shift, 0.0, masked_score)
        tile = jnp.where(before, masked_score, far_hidden)
        for h in range(per_group):
            edge[h * PAIR : (h + 1) * PAIR, :] = tile
        for l in range(layers):
            part = table[l]
            turned = jnp.dot(
                part[:, 1:] - part[:, near:], flip, precision=lax.Precision.HIGHEST,
                preferred_element_type=jnp.float32,
            )
            base = jnp.concatenate([turned, jnp.zeros((heads, PAIR), jnp.float32)], axis=1)
            for h in range(heads):
                spread = jnp.broadcast_to(base[h : h + 1], (PAIR, base.shape[1]))
                shifted = pltpu.roll(spread, 0, 1, stride=1, stride_axis=0)
                first = h % per_group * PAIR
                span = slice(first, first + PAIR)
                bias[l, h // per_group, span, :PAIR] = shifted[:, :PAIR]
                bias[l, h // per_group, span, PAIR:] = jnp.where(
                    later, masked_score, shifted[:, PAIR : 2 * PAIR]
                )

    even = lax.rem(sp, 2) == 0
    odd_behind = (lax.rem(sp, 2) == 1) & (sp >= 2)

    def halo_copy(l, c, from_slot, to_slot, index, target):
        return pltpu.make_async_remote_copy(
            src_ref=kvx.at[l, pl.ds(from_slot * rows + c * piece, piece)],
            dst_ref=kvx.at[l, pl.ds(to_slot * rows + c * piece, piece)],
            send_sem=kvs.at[l, c, index],
            recv_sem=kvr.at[l, c, to_slot],
            device_id={"sp": target},
            device_id_type=MESH,
        )

    def is_relayed(c):
        return relayed and c < CHUNKS - DIRECT

    def direct_copies(l, c):
        out_list = []
        for d in range(shift, 0, -1):
            ok = sp + d < n_sp
            if is_relayed(c) and d == 1:
                ok = even
            out_list.append((ok, halo_copy(l, c, shift, shift - d, d - 1, sp + d)))
        return out_list

    def relay_copy(l, c):
        return halo_copy(l, c, 0, 1, shift, sp - 1)

    def halo_send(l, c):
        for ok, copy in direct_copies(l, c):
            pl.when(ok)(copy.start)

    def halo_wait_slot(l, c, d):
        @pl.when(sp >= d)
        def _():
            slot = shift - d
            halo_copy(l, c, slot, slot, 0, lax.rem(sp + 1, n_sp)).wait_recv()

    def halo_far(l, c):
        halo_wait_slot(l, c, shift)
        if is_relayed(c):
            pl.when(odd_behind)(relay_copy(l, c).start)

    def halo_near(l):
        for c in range(CHUNKS):
            for d in range(shift - 1, 0, -1):
                halo_wait_slot(l, c, d)

    def wait_gain():
        own_gain.wait()
        for d in range(1, n_tp):
            pltpu.make_async_remote_copy(
                src_ref=gain,
                dst_ref=gg.at[lax.rem(tp - d + n_tp, n_tp)],
                send_sem=gs.at[d - 1],
                recv_sem=gr.at[d - 1],
                device_id={"tp": lax.rem(tp + d, n_tp)},
                device_id_type=MESH,
            ).wait_recv()

    lane = lax.broadcasted_iota(jnp.int32, (PAIR, LANES), 1) // head_dim
    scale = head_dim ** (-0.5)

    def normalize(l, c):
        span = slice(c * piece, (c + 1) * piece)
        squares = jnp.zeros((piece, 1), jnp.float32)
        for j in range(n_tp):
            part = xg[l, j, span, :].astype(jnp.float32)
            squares = squares + jnp.sum(part * part, axis=-1, keepdims=True)
        inverse = lax.rsqrt(squares / total_width + epsilon)
        for j in range(n_tp):
            part = xg[l, j, span, :].astype(jnp.float32) * inverse
            normed[span, j * width : (j + 1) * width] = (
                part * gg[j, l : l + 1, :]
            ).astype(jnp.bfloat16)

    def block_rows(b):
        return slice(b * PAIR, (b + 1) * PAIR)

    def keys_values(l, c):
        if c == 0:
            weights[l][0].wait()
            weights[l][1].wait()
        span = slice(c * piece, (c + 1) * piece)
        made = jnp.dot(normed[span, :], wkv[l], preferred_element_type=jnp.float32)
        first = REACH + c * piece
        kvx[l, first : first + piece, :] = made.astype(jnp.bfloat16)
        halo_send(l, c)

    def queries(l, b):
        if b == 0:
            weights[l][2].wait()
        qx[block_rows(b), :] = (
            jnp.dot(normed[block_rows(b), :], wq[l], preferred_element_type=jnp.float32) * scale
        ).astype(jnp.bfloat16)

    def scored(l, b, g, spans):
        lanes = slice(g * LANES, (g + 1) * LANES)
        block = qx[block_rows(b), lanes]
        stacked = jnp.concatenate(
            [jnp.where(lane == h, block, jnp.zeros_like(block)) for h in range(per_group)], axis=0
        )
        values_at = slice(head_cols + g * LANES, head_cols + (g + 1) * LANES)
        keys = jnp.concatenate([kvx[l, first:last, lanes] for first, last in spans], axis=0)
        values = jnp.concatenate([kvx[l, first:last, values_at] for first, last in spans], axis=0)
        scores = lax.dot_general(
            stacked, keys, (((1,), (1,)), ((), ())), preferred_element_type=jnp.float32
        )
        tiles = []
        starts = [at for first, last in spans for at in range(first, last, PAIR)]
        for t, at in enumerate(starts):
            tile = scores[:, t * PAIR : (t + 1) * PAIR]
            place = at // PAIR - b
            if place == 0:
                tile = tile + edge[...]
            elif at < REACH:
                behind = shift - at // rows
                tile = tile + jnp.where(sp >= behind, 0.0, masked_score)
            last_tiles = place - (BAND // PAIR - 2)
            if last_tiles >= 0:
                tile = tile + bias[l, g, :, last_tiles * PAIR : (last_tiles + 1) * PAIR]
            tiles.append(tile)
        top = jnp.max(functools.reduce(jnp.maximum, tiles), axis=-1, keepdims=True)
        return tiles, top, values

    def weighed(tiles, top, values):
        grown = [jnp.exp(tile - top) for tile in tiles]
        summed = jnp.sum(functools.reduce(jnp.add, grown), axis=-1, keepdims=True)
        packed = jnp.concatenate([tile.astype(jnp.bfloat16) for tile in grown], axis=1)
        return summed, jnp.dot(packed, values, preferred_element_type=jnp.float32)

    def attend_first(l, b, g):
        unit = b * groups + g
        spans = ((b * PAIR, rows), (REACH, REACH + (b + 1) * PAIR))
        tiles, top, values = scored(l, b, g, spans)
        summed, mix = weighed(tiles, top, values)
        top_s[unit] = top
        sum_s[unit] = summed
        mix_s[unit] = mix

    def attend_rest(l, b, g):
        unit = b * groups + g
        summed, mix = sum_s[unit], mix_s[unit]
        if shift > 1:
            tiles, top, values = scored(l, b, g, ((rows, REACH),))
            before = top_s[unit]
            top = jnp.maximum(top, before)
            more, extra = weighed(tiles, top, values)
            fade = jnp.exp(before - top)
            summed = summed * fade + more
            mix = mix * fade + extra
        mix = mix * (1.0 / summed)
        chosen = mix[:PAIR]
        for h in range(1, per_group):
            chosen = jnp.where(lane == h, mix[h * PAIR : (h + 1) * PAIR], chosen)
        att[l, tp, unit] = chosen.astype(jnp.bfloat16)

    def mixed_part(l, b, j):
        mat = wo[l, pl.ds(pl.multiple_of(j * head_cols, LANES), head_cols), :]
        left = jnp.concatenate([att[l, j, b * groups + g] for g in range(groups)], axis=1)
        return jnp.dot(left, mat, preferred_element_type=jnp.float32)

    def relay_on(gather, parts, which):
        @pl.when(core == which)
        def _():
            for part in parts:
                gather.relay(part)

    with jax.named_scope("bias"):
        make_bias()
    with jax.named_scope("gain"):
        wait_gain()

    for l in range(layers):
        gather = xgather[l]
        with jax.named_scope(f"L{l}xrel0"):
            gather.relay(0)
        for c in range(CHUNKS):
            with jax.named_scope(f"L{l}xwait{c}"):
                if c + 1 < CHUNKS:
                    relay_on(gather, (c + 1,), 1)
                gather.wait_rest(c)
            with jax.named_scope(f"L{l}norm{c}"):
                normalize(l, c)
            with jax.named_scope(f"L{l}kv{c}"):
                keys_values(l, c)
            with jax.named_scope(f"L{l}xrel{c+1}"):
                if c + 1 < CHUNKS:
                    relay_on(gather, (c + 1,), 0)
        for c in range(CHUNKS):
            with jax.named_scope(f"L{l}far{c}"):
                halo_far(l, c)
            if c < blocks:
                with jax.named_scope(f"L{l}q{c}"):
                    queries(l, c)
        for b in range(min(CHUNKS, blocks), blocks):
            queries(l, b)
        with jax.named_scope(f"L{l}attA"):
            for b in range(blocks):
                for g in range(groups):
                    attend_first(l, b, g)
        with jax.named_scope(f"L{l}near"):
            halo_near(l)
        with jax.named_scope(f"L{l}attB"):
            for b in range(blocks):
                for g in range(groups):
                    attend_rest(l, b, g)
                    agather[l].send(b * groups + g)

        gather = agather[l]
        parts = [[b * groups + g for g in range(groups)] for b in range(blocks)]
        with jax.named_scope(f"L{l}arel0"):
            weights[l][3].wait()
            for part in parts[0]:
                gather.relay(part)
        for b in range(blocks):
            with jax.named_scope(f"L{l}own{b}"):
                total = xg[l, tp, block_rows(b), :].astype(jnp.float32) + mixed_part(l, b, tp)
                for s in range(1, gather.n_x):
                    total = total + mixed_part(l, b, gather.across(s, gather.core))
            if b + 1 < blocks:
                with jax.named_scope(f"L{l}arel{b+1}n"):
                    relay_on(gather, parts[b + 1], 1)
            for i, origin in enumerate(gather.others()):
                with jax.named_scope(f"L{l}await{b}{i}"):
                    for part in parts[b]:
                        gather.wait_slot(part, origin)
                total = total + mixed_part(l, b, origin)
            with jax.named_scope(f"L{l}res{b}"):
                result = total.astype(jnp.bfloat16)
                if l + 1 < layers:
                    xg[l + 1, tp, block_rows(b), :] = result
                    for c in range(b * per_block, (b + 1) * per_block):
                        xgather[l + 1].send(c)
                else:
                    out[block_rows(b), :] = result
            if b + 1 < blocks:
                with jax.named_scope(f"L{l}arel{b+1}s"):
                    relay_on(gather, parts[b + 1], 0)

    with jax.named_scope("drain"):
        for copy in gain_copies:
            copy.wait_send()
        for l in range(layers):
            for c in range(CHUNKS):
                xgather[l].finish(c)
                for ok, copy in direct_copies(l, c):
                    pl.when(ok)(copy.wait_send)
                if is_relayed(c):
                    pl.when(odd_behind)(relay_copy(l, c).wait_send)
            for part in range(blocks * groups):
                agather[l].finish(part)


def per_device(n_tp, n_sp, stream, norm_gain, query_weight, key_weight, value_weight, out_weight, rel_bias):
    rows, width = stream.shape
    layers, full, head_cols = query_weight.shape
    heads_here = rel_bias.shape[1]
    head_dim = head_cols // heads_here
    groups = head_cols // LANES
    n_x = n_tp // 2
    shift = REACH // rows
    blocks = rows // PAIR
    tall = (LANES // head_dim) * PAIR
    any_space = pl.BlockSpec(memory_space=pltpu.HBM)
    vmem = pl.BlockSpec(memory_space=pltpu.VMEM)
    bf16, f32 = jnp.bfloat16, jnp.float32
    dma = pltpu.SemaphoreType.DMA
    operands = (stream, norm_gain, query_weight, key_weight, value_weight, out_weight, rel_bias)
    return pl.pallas_call(
        functools.partial(kernel, n_tp, n_sp, head_dim),
        out_shape=jax.ShapeDtypeStruct((rows, width), bf16),
        in_specs=[any_space] * 7,
        out_specs=vmem,
        scratch_shapes=[
            pltpu.VMEM((layers, n_tp, rows, width), bf16),
            pltpu.VMEM((n_tp, layers, width), f32),
            pltpu.VMEM(rel_bias.shape, f32),
            pltpu.VMEM((layers, full, 2 * head_cols), bf16),
            pltpu.VMEM((layers, full, head_cols), bf16),
            pltpu.VMEM((layers, n_tp * head_cols, width), bf16),
            pltpu.VMEM((rows, full), bf16),
            pltpu.VMEM((layers, groups, tall, 2 * PAIR), f32),
            pltpu.VMEM((tall, PAIR), f32),
            pltpu.VMEM((rows, head_cols), bf16),
            pltpu.VMEM((layers, REACH + rows, 2 * head_cols), bf16),
            pltpu.VMEM((layers, n_tp, blocks * groups, PAIR, LANES), bf16),
            pltpu.VMEM((blocks * groups, tall, 1), f32),
            pltpu.VMEM((blocks * groups, tall, 1), f32),
            pltpu.VMEM((blocks * groups, tall, LANES), f32),
            dma((layers, CHUNKS, 2 * n_x - 1)),
            dma((layers, CHUNKS, n_tp)),
            dma((layers, blocks * groups, 2 * n_x - 1)),
            dma((layers, blocks * groups, n_tp)),
            dma((layers, CHUNKS, shift + 1)),
            dma((layers, CHUNKS, shift)),
            dma((n_tp - 1,)),
            dma((n_tp - 1,)),
            dma((layers, 4)),
            dma((3,)),
        ],
        compiler_params=pltpu.CompilerParams(
            collective_id=0, has_side_effects=True, vmem_limit_bytes=40 * 1024 * 1024
        ),
    )(*[pltpu.with_memory_space_constraint(a, pltpu.HBM) for a in operands])


def solution(mesh):
    placed = (
        P("sp", "tp"),
        P(None, "tp"),
        P(None, None, "tp"),
        P(None, None, "tp"),
        P(None, None, "tp"),
        P(None, None, "tp"),
        P(None, "tp", None),
    )
    return jax.shard_map(
        functools.partial(per_device, mesh.shape["tp"], mesh.shape["sp"]),
        mesh=mesh, in_specs=placed, out_specs=P("sp", "tp"), check_vma=False,
    )
```

```python
import functools

import jax
import jax.numpy as jnp
from jax import lax
from jax.experimental import pallas as pl
from jax.experimental.pallas import tpu as pltpu
from jax.sharding import PartitionSpec as P

SEG = 64
PREV = 8
CLIP = 128
LANES = 128
CHUNKS = 4
PIECES = 8
EARLY = 1
LATE = 128
PAIR = 2 * SEG
REACH = PREV * SEG
BAND = REACH + PAIR

epsilon = 1e-06
masked_score = -1e30
MESH = pl.DeviceIdType.MESH


class Gather:
    def __init__(self, n_tp, slot, send_sems, recv_sems):
        self.n_x = n_tp // 2
        self.me = lax.axis_index("tp")
        self.core = lax.rem(self.me, 2)
        self.x = self.me // 2
        self.sibling = self.me + 1 - 2 * self.core
        self.slot, self.send_sems, self.recv_sems = slot, send_sems, recv_sems

    def across(self, step, core):
        return lax.rem(self.x + step, self.n_x) * 2 + core

    def outside(self):
        return [self.across(s, core) for s in range(1, self.n_x) for core in (1, 0)]

    def copy(self, origin, part, index, target):
        return pltpu.make_async_remote_copy(
            src_ref=self.slot(origin, part),
            dst_ref=self.slot(origin, part),
            send_sem=self.send_sems.at[part, index],
            recv_sem=self.recv_sems.at[part, origin],
            device_id={"tp": target},
            device_id_type=MESH,
        )

    def own(self, part):
        targets = [self.sibling] + [self.across(s, 1) for s in range(1, self.n_x)]
        return [self.copy(self.me, part, i, t) for i, t in enumerate(targets)]

    def send(self, part):
        for copy in self.own(part):
            copy.start()

    def relays(self, part):
        return [
            self.copy(origin, part, self.n_x + i, self.sibling)
            for i, origin in enumerate(self.outside())
        ]

    def relay(self, part):
        @pl.when(self.core == 1)
        def _():
            for copy in self.relays(part):
                copy.wait_recv()
                copy.start()

    def wait_slot(self, part, origin):
        self.copy(origin, part, 0, self.sibling).wait_recv()

    def wait_rest(self, part):
        self.wait_slot(part, self.sibling)

        @pl.when(self.core == 0)
        def _():
            for origin in self.outside():
                self.wait_slot(part, origin)

    def finish(self, part):
        for copy in self.own(part):
            copy.wait_send()

        @pl.when(self.core == 1)
        def _():
            for copy in self.relays(part):
                copy.wait_send()


def kernel(
    n_tp, n_sp, head_dim,
    stream, gain, query_w, key_w, value_w, out_w, rel_bias,
    out,
    xg, gg, table, wkv, wq, wo, normed, bias, edge, qx, kvx, att, top_s, mix_s,
    xs, xr, ats, atr, kvs, kvr, gs, gr, wsem, own_sem,
):
    layers, _, rows, width = xg.shape
    head_cols = qx.shape[1]
    groups = head_cols // LANES
    per_group = LANES // head_dim
    total_width = n_tp * width
    shift = REACH // rows
    sp = lax.axis_index("sp")
    tp = lax.axis_index("tp")
    relayed = shift == 2 and n_sp % 2 == 0
    blocks = rows // PAIR
    piece = rows // CHUNKS
    per_block = CHUNKS // blocks
    strip = rows // PIECES
    per_chunk = PIECES // CHUNKS
    heads = per_group * groups
    tall = per_group * PAIR

    key_cols, value_cols = slice(0, head_cols), slice(head_cols, 2 * head_cols)
    weights = []
    for l in range(layers):
        pairs = (
            (key_w, wkv.at[l, :, key_cols]),
            (value_w, wkv.at[l, :, value_cols]),
            (query_w, wq.at[l]),
            (out_w, wo.at[l]),
        )
        weights.append(
            [pltpu.make_async_copy(s.at[l], d, wsem.at[l, i]) for i, (s, d) in enumerate(pairs)]
        )
    own_stream = pltpu.make_async_copy(stream, xg.at[0, tp], own_sem.at[0])
    own_gain = pltpu.make_async_copy(gain, gg.at[tp], own_sem.at[1])
    own_stream.start()
    own_gain.start()
    own_table = pltpu.make_async_copy(rel_bias, table, own_sem.at[2])
    own_table.start()

    barrier = pltpu.get_barrier_semaphore()
    for d in range(1, n_tp):
        pl.semaphore_signal(
            barrier, inc=1, device_id={"tp": lax.rem(tp + d, n_tp)}, device_id_type=MESH
        )
    count = n_tp - 1
    even = lax.rem(sp, 2) == 0
    odd_behind = (lax.rem(sp, 2) == 1) & (sp >= 2)
    for d in range(1, shift + 1):
        pair = even if relayed and d == 1 else sp >= 0
        ahead = (sp + d < n_sp) & pair
        behind = (sp >= d) & (~even if relayed and d == 1 else sp >= 0)

        @pl.when(ahead)
        def _():
            pl.semaphore_signal(barrier, inc=1, device_id={"sp": sp + d}, device_id_type=MESH)

        @pl.when(behind)
        def _():
            pl.semaphore_signal(barrier, inc=1, device_id={"sp": sp - d}, device_id_type=MESH)

        count = count + jnp.where(ahead, 1, 0) + jnp.where(behind, 1, 0)
    for copy in weights[0]:
        copy.start()
    with jax.named_scope("barrier"):
        pl.semaphore_wait(barrier, count)

    xgather = [
        Gather(
            n_tp,
            lambda j, c, l=l: xg.at[l, j, pl.ds(c * piece, piece)],
            xs.at[l],
            xr.at[l],
        )
        for l in range(layers)
    ]
    agather = [
        Gather(n_tp, lambda j, p, l=l: att.at[l, j, p], ats.at[l], atr.at[l])
        for l in range(layers)
    ]

    gain_copies = [
        pltpu.make_async_remote_copy(
            src_ref=gg.at[tp],
            dst_ref=gg.at[tp],
            send_sem=gs.at[d - 1],
            recv_sem=gr.at[d - 1],
            device_id={"tp": lax.rem(tp + d, n_tp)},
            device_id_type=MESH,
        )
        for d in range(1, n_tp)
    ]
    own_gain.wait()
    for copy in gain_copies:
        copy.start()
    own_stream.wait()
    for c in range(CHUNKS):
        xgather[0].send(c)
    for l in range(1, layers):
        for copy in weights[l]:
            copy.start()

    for l in range(layers):
        for d in range(1, shift + 1):

            @pl.when(sp < d)
            def _():
                kvx[l, pl.ds((shift - d) * rows, rows), :] = jnp.zeros(
                    (rows, 2 * head_cols), jnp.bfloat16
                )

    near = 2 * CLIP

    def make_bias():
        own_table.wait()
        flip = (
            lax.broadcasted_iota(jnp.int32, (near, near), 0)
            + lax.broadcasted_iota(jnp.int32, (near, near), 1)
            == near - 1
        ).astype(jnp.float32)
        q_row = lax.broadcasted_iota(jnp.int32, (PAIR, PAIR), 0)
        k_col = lax.broadcasted_iota(jnp.int32, (PAIR, PAIR), 1)
        later = (q_row < SEG) & (k_col >= SEG)
        before = (q_row >= SEG) & (k_col < SEG)
        far_hidden = jnp.where(sp >= shift, 0.0, masked_score)
        tile = jnp.where(before, masked_score, far_hidden)
        for h in range(per_group):
            edge[h * PAIR : (h + 1) * PAIR, :] = tile
        for l in range(layers):
            part = table[l]
            turned = jnp.dot(
                part[:, 1:] - part[:, near:], flip, precision=lax.Precision.HIGHEST,
                preferred_element_type=jnp.float32,
            )
            base = jnp.concatenate([turned, jnp.zeros((heads, PAIR), jnp.float32)], axis=1)
            for h in range(heads):
                spread = jnp.broadcast_to(base[h : h + 1], (PAIR, base.shape[1]))
                shifted = pltpu.roll(spread, 0, 1, stride=1, stride_axis=0)
                first = h % per_group * PAIR
                span = slice(first, first + PAIR)
                bias[l, h // per_group, span, :PAIR] = shifted[:, :PAIR]
                bias[l, h // per_group, span, PAIR:] = jnp.where(
                    later, masked_score, shifted[:, PAIR : 2 * PAIR]
                )

    def halo_copy(l, c, from_slot, to_slot, index, target):
        return pltpu.make_async_remote_copy(
            src_ref=kvx.at[l, pl.ds(from_slot * rows + c * strip, strip)],
            dst_ref=kvx.at[l, pl.ds(to_slot * rows + c * strip, strip)],
            send_sem=kvs.at[l, c, index],
            recv_sem=kvr.at[l, c, to_slot],
            device_id={"sp": target},
            device_id_type=MESH,
        )

    def direct_copies(l, c):
        out_list = []
        for d in range(shift, 0, -1):
            ok = sp + d < n_sp
            if relayed and d == 1:
                ok = even & ok
            out_list.append((ok, halo_copy(l, c, shift, shift - d, d - 1, sp + d)))
        return out_list

    def relay_copy(l, c):
        return halo_copy(l, c, 0, 1, shift, sp - 1)

    def halo_send(l, c):
        for ok, copy in direct_copies(l, c):
            pl.when(ok)(copy.start)

    def halo_wait_slot(l, c, d):
        @pl.when(sp >= d)
        def _():
            slot = shift - d
            halo_copy(l, c, slot, slot, 0, lax.rem(sp + 1, n_sp)).wait_recv()

    def halo_relay(l, c):
        @pl.when(odd_behind)
        def _():
            halo_copy(l, c, 0, 0, 0, lax.rem(sp + 1, n_sp)).wait_recv()
            relay_copy(l, c).start()

    def halo_far(l, c):
        if relayed:

            @pl.when(even & (sp >= 2))
            def _():
                halo_copy(l, c, 0, 0, 0, lax.rem(sp + 1, n_sp)).wait_recv()

        else:
            halo_wait_slot(l, c, shift)

    def halo_near(l, pieces):
        for c in pieces:
            for d in range(shift - 1, 0, -1):
                halo_wait_slot(l, c, d)

    def wait_gain():
        for d in range(1, n_tp):
            pltpu.make_async_remote_copy(
                src_ref=gg.at[tp],
                dst_ref=gg.at[lax.rem(tp - d + n_tp, n_tp)],
                send_sem=gs.at[d - 1],
                recv_sem=gr.at[d - 1],
                device_id={"tp": lax.rem(tp + d, n_tp)},
                device_id_type=MESH,
            ).wait_recv()

    lane = lax.broadcasted_iota(jnp.int32, (PAIR, LANES), 1) // head_dim
    scale = head_dim ** (-0.5)

    def normalize(l, c):
        span = slice(c * piece, (c + 1) * piece)
        squares = jnp.zeros((piece, 1), jnp.float32)
        for j in range(n_tp):
            part = xg[l, j, span, :].astype(jnp.float32)
            squares = squares + jnp.sum(part * part, axis=-1, keepdims=True)
        inverse = lax.rsqrt(squares / total_width + epsilon)
        for j in range(n_tp):
            part = xg[l, j, span, :].astype(jnp.float32) * inverse
            normed[span, j * width : (j + 1) * width] = (
                part * gg[j, l : l + 1, :]
            ).astype(jnp.bfloat16)

    def block_rows(b):
        return slice(b * PAIR, (b + 1) * PAIR)

    def keys_values(l, c):
        if c == 0:
            weights[l][0].wait()
            weights[l][1].wait()
        span = slice(c * piece, (c + 1) * piece)
        made = jnp.dot(normed[span, :], wkv[l], preferred_element_type=jnp.float32)
        first = REACH + c * piece
        kvx[l, first : first + piece, :] = made.astype(jnp.bfloat16)
        for p in range(c * per_chunk, (c + 1) * per_chunk):
            halo_send(l, p)

    def queries(l, b):
        if b == 0:
            weights[l][2].wait()
        qx[block_rows(b), :] = (
            jnp.dot(normed[block_rows(b), :], wq[l], preferred_element_type=jnp.float32) * scale
        ).astype(jnp.bfloat16)

    def scored(l, b, g, spans):
        lanes = slice(g * LANES, (g + 1) * LANES)
        block = qx[block_rows(b), lanes]
        stacked = jnp.concatenate(
            [jnp.where(lane == h, block, jnp.zeros_like(block)) for h in range(per_group)], axis=0
        )
        values_at = slice(head_cols + g * LANES, head_cols + (g + 1) * LANES)
        keys = jnp.concatenate([kvx[l, first:last, lanes] for first, last in spans], axis=0)
        values = jnp.concatenate([kvx[l, first:last, values_at] for first, last in spans], axis=0)
        scores = lax.dot_general(
            stacked, keys, (((1,), (1,)), ((), ())), preferred_element_type=jnp.float32
        )
        tiles = []
        starts = [at for first, last in spans for at in range(first, last, PAIR)]
        for t, at in enumerate(starts):
            tile = scores[:, t * PAIR : (t + 1) * PAIR]
            place = at // PAIR - b
            if place == 0:
                tile = tile + edge[...]
            elif at < REACH:
                behind = shift - at // rows
                tile = tile + jnp.where(sp >= behind, 0.0, masked_score)
            last_tiles = place - (BAND // PAIR - 2)
            if last_tiles >= 0:
                tile = tile + bias[l, g, :, last_tiles * PAIR : (last_tiles + 1) * PAIR]
            tiles.append(tile)
        top = jnp.max(functools.reduce(jnp.maximum, tiles), axis=-1, keepdims=True)
        return tiles, jnp.broadcast_to(top, (tall, LANES)), values

    def weighed(tiles, top, values):
        packed = jnp.concatenate([jnp.exp(tile - top).astype(jnp.bfloat16) for tile in tiles], axis=1)
        beside = jnp.concatenate([values, jnp.ones_like(values)], axis=1)
        return jnp.dot(packed, beside, preferred_element_type=jnp.float32)

    def attend_first(l, b, g):
        unit = b * groups + g
        spans = ((b * PAIR, rows), (rows, REACH - LATE), (REACH, REACH + (b + 1) * PAIR))
        tiles, top, values = scored(l, b, g, [s for s in spans if s[1] > s[0]])
        top_s[unit] = top
        mix_s[unit] = weighed(tiles, top, values)

    def attend_rest(l, b, g):
        unit = b * groups + g
        tiles, top, values = scored(l, b, g, ((REACH - LATE, REACH),))
        before = top_s[unit]
        top = jnp.maximum(top, before)
        fade = jnp.exp(before - top)
        mix = mix_s[unit] * jnp.concatenate([fade, fade], axis=1) + weighed(tiles, top, values)
        mix = mix[:, :LANES] / mix[:, LANES:]
        chosen = mix[:PAIR]
        for h in range(1, per_group):
            chosen = jnp.where(lane == h, mix[h * PAIR : (h + 1) * PAIR], chosen)
        att[l, tp, unit] = chosen.astype(jnp.bfloat16)

    def mixed_part(l, b, j):
        mat = wo[l, pl.ds(pl.multiple_of(j * head_cols, LANES), head_cols), :]
        left = jnp.concatenate([att[l, j, b * groups + g] for g in range(groups)], axis=1)
        return jnp.dot(left, mat, preferred_element_type=jnp.float32)

    with jax.named_scope("bias"):
        make_bias()
    with jax.named_scope("gain"):
        wait_gain()

    for l in range(layers):
        gather = xgather[l]
        for c in range(CHUNKS):
            with jax.named_scope(f"L{l}xrel{c}"):
                gather.relay(c)
            with jax.named_scope(f"L{l}xwait{c}"):
                gather.wait_rest(c)
            with jax.named_scope(f"L{l}norm{c}"):
                normalize(l, c)
            with jax.named_scope(f"L{l}kv{c}"):
                keys_values(l, c)
            if relayed and c + 2 == CHUNKS:
                with jax.named_scope(f"L{l}hrel0"):
                    for p in range(EARLY):
                        halo_relay(l, p)
        for b in range(blocks):
            for p in range(EARLY + b, EARLY + b + 1):
                if relayed:
                    with jax.named_scope(f"L{l}hrel{p}"):
                        halo_relay(l, p)
            with jax.named_scope(f"L{l}q{b}"):
                queries(l, b)
        if relayed:
            for p in range(EARLY + blocks, PIECES):
                with jax.named_scope(f"L{l}hrel{p}"):
                    halo_relay(l, p)
        split = (REACH - LATE - (shift - 1) * rows) // strip
        with jax.named_scope(f"L{l}far"):
            for p in range(PIECES):
                halo_far(l, p)
        with jax.named_scope(f"L{l}near0"):
            halo_near(l, range(split))
        with jax.named_scope(f"L{l}attA"):
            for b in range(blocks):
                for g in range(groups):
                    attend_first(l, b, g)
        with jax.named_scope(f"L{l}near"):
            halo_near(l, range(split, PIECES))
        with jax.named_scope(f"L{l}attB"):
            for b in range(blocks):
                for g in range(groups):
                    attend_rest(l, b, g)
                for g in range(groups):
                    agather[l].send(b * groups + g)

        gather = agather[l]
        parts = [[b * groups + g for g in range(groups)] for b in range(blocks)]
        weights[l][3].wait()
        for b in range(blocks):
            with jax.named_scope(f"L{l}own{b}"):
                total = xg[l, tp, block_rows(b), :].astype(jnp.float32) + mixed_part(l, b, tp)
            with jax.named_scope(f"L{l}arel{b}"):
                for part in parts[b]:
                    gather.relay(part)
            with jax.named_scope(f"L{l}await{b}"):
                for part in parts[b]:
                    gather.wait_rest(part)
            with jax.named_scope(f"L{l}res{b}"):
                for origin in [gather.sibling] + gather.outside():
                    total = total + mixed_part(l, b, origin)
                result = total.astype(jnp.bfloat16)
                if l + 1 < layers:
                    xg[l + 1, tp, block_rows(b), :] = result
                    for c in range(b * per_block, (b + 1) * per_block):
                        xgather[l + 1].send(c)
                else:
                    out[block_rows(b), :] = result

    with jax.named_scope("drain"):
        for copy in gain_copies:
            copy.wait_send()
        for l in range(layers):
            for c in range(CHUNKS):
                xgather[l].finish(c)
            for p in range(PIECES):
                for ok, copy in direct_copies(l, p):
                    pl.when(ok)(copy.wait_send)
                if relayed:
                    pl.when(odd_behind)(relay_copy(l, p).wait_send)
            for part in range(blocks * groups):
                agather[l].finish(part)


def per_device(n_tp, n_sp, stream, norm_gain, query_weight, key_weight, value_weight, out_weight, rel_bias):
    rows, width = stream.shape
    layers, full, head_cols = query_weight.shape
    heads_here = rel_bias.shape[1]
    head_dim = head_cols // heads_here
    groups = head_cols // LANES
    n_x = n_tp // 2
    shift = REACH // rows
    blocks = rows // PAIR
    tall = (LANES // head_dim) * PAIR
    any_space = pl.BlockSpec(memory_space=pltpu.HBM)
    vmem = pl.BlockSpec(memory_space=pltpu.VMEM)
    bf16, f32 = jnp.bfloat16, jnp.float32
    dma = pltpu.SemaphoreType.DMA
    operands = (stream, norm_gain, query_weight, key_weight, value_weight, out_weight, rel_bias)
    return pl.pallas_call(
        functools.partial(kernel, n_tp, n_sp, head_dim),
        out_shape=jax.ShapeDtypeStruct((rows, width), bf16),
        in_specs=[any_space] * 7,
        out_specs=vmem,
        scratch_shapes=[
            pltpu.VMEM((layers, n_tp, rows, width), bf16),
            pltpu.VMEM((n_tp, layers, width), f32),
            pltpu.VMEM(rel_bias.shape, f32),
            pltpu.VMEM((layers, full, 2 * head_cols), bf16),
            pltpu.VMEM((layers, full, head_cols), bf16),
            pltpu.VMEM((layers, n_tp * head_cols, width), bf16),
            pltpu.VMEM((rows, full), bf16),
            pltpu.VMEM((layers, groups, tall, 2 * PAIR), f32),
            pltpu.VMEM((tall, PAIR), f32),
            pltpu.VMEM((rows, head_cols), bf16),
            pltpu.VMEM((layers, REACH + rows, 2 * head_cols), bf16),
            pltpu.VMEM((layers, n_tp, blocks * groups, PAIR, LANES), bf16),
            pltpu.VMEM((blocks * groups, tall, LANES), f32),
            pltpu.VMEM((blocks * groups, tall, 2 * LANES), f32),
            dma((layers, CHUNKS, 3 * n_x - 2)),
            dma((layers, CHUNKS, n_tp)),
            dma((layers, blocks * groups, 3 * n_x - 2)),
            dma((layers, blocks * groups, n_tp)),
            dma((layers, PIECES, shift + 1)),
            dma((layers, PIECES, shift)),
            dma((n_tp - 1,)),
            dma((n_tp - 1,)),
            dma((layers, 4)),
            dma((3,)),
        ],
        compiler_params=pltpu.CompilerParams(
            collective_id=0, has_side_effects=True, vmem_limit_bytes=40 * 1024 * 1024
        ),
    )(*[pltpu.with_memory_space_constraint(a, pltpu.HBM) for a in operands])


def solution(mesh):
    placed = (
        P("sp", "tp"),
        P(None, "tp"),
        P(None, None, "tp"),
        P(None, None, "tp"),
        P(None, None, "tp"),
        P(None, None, "tp"),
        P(None, "tp", None),
    )
    return jax.shard_map(
        functools.partial(per_device, mesh.shape["tp"], mesh.shape["sp"]),
        mesh=mesh, in_specs=placed, out_specs=P("sp", "tp"), check_vma=False,
    )
```

```python
import functools

import jax
import jax.numpy as jnp
from jax import lax
from jax.experimental import pallas as pl
from jax.experimental.pallas import tpu as pltpu
from jax.sharding import PartitionSpec as P

SEG = 64
PREV = 8
CLIP = 128
LANES = 128
STRIP = 32
CHUNK = 64
FIRST = 64
EARLY = 1
PAIR = 2 * SEG
REACH = PREV * SEG
BAND = REACH + PAIR

epsilon = 1e-06
masked_score = -1e30
MESH = pl.DeviceIdType.MESH


class Gather:
    def __init__(self, n_tp, buf, layer, spans, send_sems, recv_sems):
        self.n_tp, self.n_x = n_tp, n_tp // 2
        self.me = lax.axis_index("tp")
        self.core = lax.rem(self.me, 2)
        self.x = self.me // 2
        self.sibling = self.me + 1 - 2 * self.core
        self.buf, self.layer, self.spans = buf, layer, spans
        self.send_sems, self.recv_sems = send_sems, recv_sems

    def across(self, step, core):
        return lax.rem(self.x + step, self.n_x) * 2 + core

    def outside(self):
        return [self.across(s, core) for s in range(1, self.n_x) for core in (1, 0)]

    def copy(self, first, count, part, index, target):
        start, stop = (0, self.buf.shape[2]) if part is None else self.spans[part]
        block = self.buf.at[self.layer, pl.ds(first, count), pl.ds(start, stop - start)]
        return pltpu.make_async_remote_copy(
            src_ref=block,
            dst_ref=block,
            send_sem=self.send_sems.at[index],
            recv_sem=self.recv_sems.at[part or 0],
            device_id={"tp": target},
            device_id_type=MESH,
        )

    def own(self, part):
        targets = [self.sibling] + [self.across(s, 1) for s in range(1, self.n_x)]
        return [self.copy(self.me, 1, part, i, t) for i, t in enumerate(targets)]

    def send(self, part):
        for copy in self.own(part):
            copy.start()

    def relays(self, part):
        return [
            self.copy(self.across(s, 0), 2, part, self.n_x + s - 1, self.sibling)
            for s in range(1, self.n_x)
        ]

    def take(self, part):
        self.copy(0, self.n_tp - 1, part, 0, self.sibling).wait_recv()

        @pl.when(self.core == 1)
        def _():
            for copy in self.relays(part):
                copy.start()

    def finish(self):
        for copy in self.own(None):
            copy.wait_send()

        @pl.when(self.core == 1)
        def _():
            for copy in self.relays(None):
                copy.wait_send()


def kernel(
    n_tp, n_sp, head_dim,
    stream, gain, query_w, key_w, value_w, out_w, rel_bias,
    out,
    xg, gg, table, wkv, wq, wo, normed, bias, edge, qx, kvx, att, top_s, mix_s,
    xs, xr, ats, atr, kvs, far_sem, near_sem, gain_sem, wsem, own_sem,
):
    layers, _, rows, width = xg.shape
    head_cols = qx.shape[1]
    groups = head_cols // LANES
    per_group = LANES // head_dim
    total_width = n_tp * width
    shift = REACH // rows
    sp = lax.axis_index("sp")
    tp = lax.axis_index("tp")
    relayed = shift == 2 and n_sp % 2 == 0
    blocks = rows // PAIR
    half = rows // 2
    cuts = [0] + list(range(FIRST, rows, CHUNK)) + [rows]
    chunks = list(zip(cuts[:-1], cuts[1:]))
    pieces = rows // STRIP
    heads = per_group * groups
    tall = per_group * PAIR

    key_cols, value_cols = slice(0, head_cols), slice(head_cols, 2 * head_cols)
    weights = []
    for l in range(layers):
        pairs = (
            (key_w, wkv.at[l, :, key_cols]),
            (value_w, wkv.at[l, :, value_cols]),
            (query_w, wq.at[l]),
            (out_w, wo.at[l]),
        )
        weights.append(
            [pltpu.make_async_copy(s.at[l], d, wsem.at[l, max(i - 1, 0)]) for i, (s, d) in enumerate(pairs)]
        )
    own_stream = pltpu.make_async_copy(stream, xg.at[0, tp], own_sem.at[0])
    own_gain = pltpu.make_async_copy(gain, gg.at[tp], own_sem.at[1])
    own_stream.start()
    own_gain.start()
    own_table = pltpu.make_async_copy(rel_bias, table, own_sem.at[2])
    own_table.start()

    barrier = pltpu.get_barrier_semaphore()
    for d in range(1, n_tp):
        pl.semaphore_signal(
            barrier, inc=1, device_id={"tp": lax.rem(tp + d, n_tp)}, device_id_type=MESH
        )
    count = n_tp - 1
    even = lax.rem(sp, 2) == 0
    odd_behind = (lax.rem(sp, 2) == 1) & (sp >= 2)
    for d in range(1, shift + 1):
        pair = even if relayed and d == 1 else sp >= 0
        ahead = (sp + d < n_sp) & pair
        behind = (sp >= d) & (~even if relayed and d == 1 else sp >= 0)

        @pl.when(ahead)
        def _():
            pl.semaphore_signal(barrier, inc=1, device_id={"sp": sp + d}, device_id_type=MESH)

        @pl.when(behind)
        def _():
            pl.semaphore_signal(barrier, inc=1, device_id={"sp": sp - d}, device_id_type=MESH)

        count = count + jnp.where(ahead, 1, 0) + jnp.where(behind, 1, 0)
    for copy in weights[0]:
        copy.start()
    with jax.named_scope("barrier"):
        pl.semaphore_wait(barrier, count)

    xgather = [Gather(n_tp, xg, l, chunks, xs, xr.at[l]) for l in range(layers)]
    units = blocks * groups
    shares = [(b * groups, (b + 1) * groups) for b in range(blocks)]
    agather = [Gather(n_tp, att, l, shares, ats, atr.at[l]) for l in range(layers)]

    gain_copies = [
        pltpu.make_async_remote_copy(
            src_ref=gg.at[tp],
            dst_ref=gg.at[tp],
            send_sem=gain_sem.at[0],
            recv_sem=gain_sem.at[1],
            device_id={"tp": lax.rem(tp + d, n_tp)},
            device_id_type=MESH,
        )
        for d in range(1, n_tp)
    ]
    other_gains = gg.at[pl.ds(0, n_tp - 1)]
    all_gains = pltpu.make_async_remote_copy(
        src_ref=other_gains,
        dst_ref=other_gains,
        send_sem=gain_sem.at[0],
        recv_sem=gain_sem.at[1],
        device_id={"tp": lax.rem(tp + 1, n_tp)},
        device_id_type=MESH,
    )
    own_gain.wait()
    for copy in gain_copies:
        copy.start()
    own_stream.wait()
    for c in range(len(chunks)):
        xgather[0].send(c)
    for l in range(1, layers):
        for copy in weights[l]:
            copy.start()

    for l in range(layers):
        for d in range(1, shift + 1):

            @pl.when(sp < d)
            def _():
                kvx[l, pl.ds((shift - d) * rows, rows), :] = jnp.zeros(
                    (rows, 2 * head_cols), jnp.bfloat16
                )

    near = 2 * CLIP

    def make_bias():
        own_table.wait()
        flip = (
            lax.broadcasted_iota(jnp.int32, (near, near), 0)
            + lax.broadcasted_iota(jnp.int32, (near, near), 1)
            == near - 1
        ).astype(jnp.float32)
        q_row = lax.broadcasted_iota(jnp.int32, (PAIR, PAIR), 0)
        k_col = lax.broadcasted_iota(jnp.int32, (PAIR, PAIR), 1)
        later = (q_row < SEG) & (k_col >= SEG)
        before = (q_row >= SEG) & (k_col < SEG)
        far_hidden = jnp.where(sp >= shift, 0.0, masked_score)
        tile = jnp.where(before, masked_score, far_hidden)
        for h in range(per_group):
            edge[h * PAIR : (h + 1) * PAIR, :] = tile
        for l in range(layers):
            part = table[l]
            turned = jnp.dot(
                part[:, 1:] - part[:, near:], flip, precision=lax.Precision.HIGHEST,
                preferred_element_type=jnp.float32,
            )
            base = jnp.concatenate([turned, jnp.zeros((heads, PAIR), jnp.float32)], axis=1)
            for h in range(heads):
                spread = jnp.broadcast_to(base[h : h + 1], (PAIR, base.shape[1]))
                shifted = pltpu.roll(spread, 0, 1, stride=1, stride_axis=0)
                first = h % per_group * PAIR
                span = slice(first, first + PAIR)
                bias[l, h // per_group, span, :PAIR] = shifted[:, :PAIR]
                bias[l, h // per_group, span, PAIR:] = jnp.where(
                    later, masked_score, shifted[:, PAIR : 2 * PAIR]
                )

    def halo_copy(l, p, from_slot, to_slot, index, target):
        first, size = (0, rows) if p is None else (p * STRIP, STRIP)
        p = p or 0
        if to_slot == 0:
            arrived = far_sem.at[l, p]
        else:
            arrived = near_sem.at[l, to_slot - 1, p * STRIP // half]
        return pltpu.make_async_remote_copy(
            src_ref=kvx.at[l, pl.ds(from_slot * rows + first, size)],
            dst_ref=kvx.at[l, pl.ds(to_slot * rows + first, size)],
            send_sem=kvs.at[index],
            recv_sem=arrived,
            device_id={"sp": target},
            device_id_type=MESH,
        )

    def direct_copies(l, p):
        out_list = []
        for d in range(shift, 0, -1):
            ok = sp + d < n_sp
            if relayed and d == 1:
                ok = even & ok
            out_list.append((ok, halo_copy(l, p, shift, shift - d, d - 1, sp + d)))
        return out_list

    def relay_copy(l, p):
        return halo_copy(l, p, 0, 1, shift, sp - 1)

    def halo_send(l, p):
        for ok, copy in direct_copies(l, p):
            pl.when(ok)(copy.start)

    def halo_finish(l):
        for ok, copy in direct_copies(l, None):
            pl.when(ok)(copy.wait_send)
        if relayed:
            pl.when(odd_behind)(relay_copy(l, None).wait_send)

    def far_wait(l, p):
        halo_copy(l, p, 0, 0, 0, lax.rem(sp + 1, n_sp)).wait_recv()

    def halo_relay(l, p):
        if relayed:

            @pl.when(odd_behind)
            def _():
                far_wait(l, p)
                relay_copy(l, p).start()

    def halo_far(l, which):
        here = sp >= shift
        if relayed:
            here = here & even

        @pl.when(here)
        def _():
            for p in range(which * half // STRIP, (which + 1) * half // STRIP):
                far_wait(l, p)

    def halo_near(l, which):
        for d in range(shift - 1, 0, -1):
            slot = shift - d

            @pl.when(sp >= d)
            def _():
                part = kvx.at[l, pl.ds(slot * rows + which * half, half)]
                pltpu.make_async_remote_copy(
                    src_ref=part,
                    dst_ref=part,
                    send_sem=kvs.at[0],
                    recv_sem=near_sem.at[l, slot - 1, which],
                    device_id={"sp": lax.rem(sp + 1, n_sp)},
                    device_id_type=MESH,
                ).wait_recv()

    lane = lax.broadcasted_iota(jnp.int32, (PAIR, LANES), 1) // head_dim
    scale = head_dim ** (-0.5)

    def normalize(l, c):
        span = slice(*chunks[c])
        squares = jnp.zeros((span.stop - span.start, 1), jnp.float32)
        for j in range(n_tp):
            part = xg[l, j, span, :].astype(jnp.float32)
            squares = squares + jnp.sum(part * part, axis=-1, keepdims=True)
        inverse = lax.rsqrt(squares / total_width + epsilon)
        for j in range(n_tp):
            part = xg[l, j, span, :].astype(jnp.float32) * inverse
            normed[span, j * width : (j + 1) * width] = (
                part * gg[j, l : l + 1, :]
            ).astype(jnp.bfloat16)

    def block_rows(b):
        return slice(b * PAIR, (b + 1) * PAIR)

    def keys_values(l, c):
        start, stop = chunks[c]
        if c == 0:
            pltpu.make_async_copy(wkv.at[l], wkv.at[l], wsem.at[l, 0]).wait()
            if l > 0:
                halo_finish(l - 1)
        made = jnp.dot(normed[start:stop, :], wkv[l], preferred_element_type=jnp.float32)
        kvx[l, REACH + start : REACH + stop, :] = made.astype(jnp.bfloat16)
        for p in range(start // STRIP, stop // STRIP):
            halo_send(l, p)

    def queries(l, b):
        if b == 0:
            weights[l][2].wait()
        qx[block_rows(b), :] = (
            jnp.dot(normed[block_rows(b), :], wq[l], preferred_element_type=jnp.float32) * scale
        ).astype(jnp.bfloat16)

    def scored(l, b, g, spans):
        lanes = slice(g * LANES, (g + 1) * LANES)
        block = qx[block_rows(b), lanes]
        stacked = jnp.concatenate(
            [jnp.where(lane == h, block, jnp.zeros_like(block)) for h in range(per_group)], axis=0
        )
        values_at = slice(head_cols + g * LANES, head_cols + (g + 1) * LANES)
        keys = jnp.concatenate([kvx[l, first:last, lanes] for first, last in spans], axis=0)
        values = jnp.concatenate([kvx[l, first:last, values_at] for first, last in spans], axis=0)
        scores = lax.dot_general(
            stacked, keys, (((1,), (1,)), ((), ())), preferred_element_type=jnp.float32
        )
        tiles = []
        starts = [at for first, last in spans for at in range(first, last, PAIR)]
        for t, at in enumerate(starts):
            tile = scores[:, t * PAIR : (t + 1) * PAIR]
            place = at // PAIR - b
            if place == 0:
                tile = tile + edge[...]
            elif at < REACH:
                behind = shift - at // rows
                tile = tile + jnp.where(sp >= behind, 0.0, masked_score)
            last_tiles = place - (BAND // PAIR - 2)
            if last_tiles >= 0:
                tile = tile + bias[l, g, :, last_tiles * PAIR : (last_tiles + 1) * PAIR]
            tiles.append(tile)
        top = jnp.max(functools.reduce(jnp.maximum, tiles), axis=-1, keepdims=True)
        return tiles, jnp.broadcast_to(top, (tall, LANES)), values

    def weighed(tiles, top, values):
        packed = jnp.concatenate([jnp.exp(tile - top).astype(jnp.bfloat16) for tile in tiles], axis=1)
        beside = jnp.concatenate([values, jnp.ones_like(values)], axis=1)
        return jnp.dot(packed, beside, preferred_element_type=jnp.float32)

    def attend_first(l, b, g):
        unit = b * groups + g
        spans = [(max(b * PAIR, at), at + half) for at in range(0, REACH, rows)]
        spans.append((REACH, REACH + (b + 1) * PAIR))
        tiles, top, values = scored(l, b, g, [s for s in spans if s[1] > s[0]])
        top_s[unit] = top
        mix_s[unit] = weighed(tiles, top, values)

    def attend_rest(l, b, g):
        unit = b * groups + g
        spans = [(max(b * PAIR, at + half), at + rows) for at in range(0, REACH, rows)]
        tiles, top, values = scored(l, b, g, spans)
        before = top_s[unit]
        top = jnp.maximum(top, before)
        fade = jnp.exp(before - top)
        mix = mix_s[unit] * jnp.concatenate([fade, fade], axis=1) + weighed(tiles, top, values)
        mix = mix[:, :LANES] / mix[:, LANES:]
        chosen = mix[:PAIR]
        for h in range(1, per_group):
            chosen = jnp.where(lane == h, mix[h * PAIR : (h + 1) * PAIR], chosen)
        att[l, tp, unit] = chosen.astype(jnp.bfloat16)

    def mixed_part(l, b, j):
        mat = wo[l, pl.ds(pl.multiple_of(j * head_cols, LANES), head_cols), :]
        left = jnp.concatenate([att[l, j, b * groups + g] for g in range(groups)], axis=1)
        return jnp.dot(left, mat, preferred_element_type=jnp.float32)

    with jax.named_scope("bias"):
        make_bias()
    with jax.named_scope("gain"):
        all_gains.wait_recv()

    for l in range(layers):
        gather = xgather[l]
        for c in range(len(chunks)):
            with jax.named_scope(f"L{l}xtake{c}"):
                gather.take(c)
            with jax.named_scope(f"L{l}norm{c}"):
                normalize(l, c)
            with jax.named_scope(f"L{l}kv{c}"):
                keys_values(l, c)
            if c + 2 == len(chunks):
                with jax.named_scope(f"L{l}hrelE"):
                    for p in range(EARLY):
                        halo_relay(l, p)
        for b in range(blocks):
            with jax.named_scope(f"L{l}hrel{EARLY+b}"):
                halo_relay(l, EARLY + b)
            with jax.named_scope(f"L{l}q{b}"):
                queries(l, b)
        turn = half // STRIP
        steps = [range(EARLY + blocks, turn)]
        if l == 0:
            spare = (pieces - turn) // blocks
            steps += [range(turn + b * spare, turn + (b + 1) * spare) for b in range(blocks)]
            steps.append(range(turn + blocks * spare, pieces))
        else:
            steps[0] = range(EARLY + blocks, pieces)
            steps += [()] * (blocks + 1)
        with jax.named_scope(f"L{l}hrelM"):
            for p in steps[0]:
                halo_relay(l, p)
        with jax.named_scope(f"L{l}far0"):
            halo_far(l, 0)
        with jax.named_scope(f"L{l}near0"):
            halo_near(l, 0)
        for b in range(blocks):
            with jax.named_scope(f"L{l}A{b}"):
                for g in range(groups):
                    attend_first(l, b, g)
            with jax.named_scope(f"L{l}hrelA{b}"):
                for p in steps[b + 1]:
                    halo_relay(l, p)
        with jax.named_scope(f"L{l}hrelZ"):
            for p in steps[-1]:
                halo_relay(l, p)
        with jax.named_scope(f"L{l}far1"):
            halo_far(l, 1)
        with jax.named_scope(f"L{l}near1"):
            halo_near(l, 1)
        if l > 0:
            agather[l - 1].finish()
        for b in range(blocks):
            with jax.named_scope(f"L{l}B{b}"):
                for g in range(groups):
                    attend_rest(l, b, g)
            agather[l].send(b)

        gather = agather[l]
        weights[l][3].wait()
        for b in range(blocks):
            with jax.named_scope(f"L{l}own{b}"):
                total = xg[l, tp, block_rows(b), :].astype(jnp.float32) + mixed_part(l, b, tp)
            with jax.named_scope(f"L{l}atake{b}"):
                gather.take(b)
            with jax.named_scope(f"L{l}res{b}"):
                for origin in [gather.sibling] + gather.outside():
                    total = total + mixed_part(l, b, origin)
                result = total.astype(jnp.bfloat16)
                if l + 1 < layers:
                    if b == 0:
                        xgather[l].finish()
                    xg[l + 1, tp, block_rows(b), :] = result
                    for c, (_, stop) in enumerate(chunks):
                        if b * PAIR < stop <= (b + 1) * PAIR:
                            xgather[l + 1].send(c)
                else:
                    out[block_rows(b), :] = result

    with jax.named_scope("drain"):
        all_gains.wait_send()
        xgather[layers - 1].finish()
        agather[layers - 1].finish()
        halo_finish(layers - 1)


def per_device(n_tp, n_sp, stream, norm_gain, query_weight, key_weight, value_weight, out_weight, rel_bias):
    rows, width = stream.shape
    layers, full, head_cols = query_weight.shape
    heads_here = rel_bias.shape[1]
    head_dim = head_cols // heads_here
    groups = head_cols // LANES
    n_x = n_tp // 2
    shift = REACH // rows
    blocks = rows // PAIR
    tall = (LANES // head_dim) * PAIR
    chunk_count = len(range(FIRST, rows, CHUNK)) + 1
    any_space = pl.BlockSpec(memory_space=pltpu.HBM)
    vmem = pl.BlockSpec(memory_space=pltpu.VMEM)
    bf16, f32 = jnp.bfloat16, jnp.float32
    dma = pltpu.SemaphoreType.DMA
    operands = (stream, norm_gain, query_weight, key_weight, value_weight, out_weight, rel_bias)
    return pl.pallas_call(
        functools.partial(kernel, n_tp, n_sp, head_dim),
        out_shape=jax.ShapeDtypeStruct((rows, width), bf16),
        in_specs=[any_space] * 7,
        out_specs=vmem,
        scratch_shapes=[
            pltpu.VMEM((layers, n_tp, rows, width), bf16),
            pltpu.VMEM((n_tp, layers, width), f32),
            pltpu.VMEM(rel_bias.shape, f32),
            pltpu.VMEM((layers, full, 2 * head_cols), bf16),
            pltpu.VMEM((layers, full, head_cols), bf16),
            pltpu.VMEM((layers, n_tp * head_cols, width), bf16),
            pltpu.VMEM((rows, full), bf16),
            pltpu.VMEM((layers, groups, tall, 2 * PAIR), f32),
            pltpu.VMEM((tall, PAIR), f32),
            pltpu.VMEM((rows, head_cols), bf16),
            pltpu.VMEM((layers, REACH + rows, 2 * head_cols), bf16),
            pltpu.VMEM((layers, n_tp, blocks * groups, PAIR, LANES), bf16),
            pltpu.VMEM((blocks * groups, tall, LANES), f32),
            pltpu.VMEM((blocks * groups, tall, 2 * LANES), f32),
            dma((2 * n_x - 1,)),
            dma((layers, chunk_count)),
            dma((2 * n_x - 1,)),
            dma((layers, blocks)),
            dma((shift + 1,)),
            dma((layers, rows // STRIP)),
            dma((layers, max(shift - 1, 1), 2)),
            dma((2,)),
            dma((layers, 3)),
            dma((3,)),
        ],
        compiler_params=pltpu.CompilerParams(
            collective_id=0, has_side_effects=True, vmem_limit_bytes=40 * 1024 * 1024
        ),
    )(*[pltpu.with_memory_space_constraint(a, pltpu.HBM) for a in operands])


def solution(mesh):
    placed = (
        P("sp", "tp"),
        P(None, "tp"),
        P(None, None, "tp"),
        P(None, None, "tp"),
        P(None, None, "tp"),
        P(None, None, "tp"),
        P(None, "tp", None),
    )
    return jax.shard_map(
        functools.partial(per_device, mesh.shape["tp"], mesh.shape["sp"]),
        mesh=mesh, in_specs=placed, out_specs=P("sp", "tp"), check_vma=False,
    )
```
